32 devices in a mesh: ep: 8 (over z, x), tp: 4 (over y, core).
Axes of the slice: x: 2, y: 2, z: 4, core: 2. Of those that a mesh axis runs over, the one named last changes fastest.
Arguments:
- mixer_input: bfloat16 [1024, 2048], P('ep'), may hold values from -6 to 6
- mixer_gain: float32 [2048], replicated, may hold values from 0.1 to 1.9
- outer_weight: bfloat16 [2048, 1024], P(None, 'tp'), may hold values from -0.125 to 0.125
- inner_weight: bfloat16 [2048, 1024], P(None, 'tp'), may hold values from -0.125 to 0.125
- value_weight: bfloat16 [2048, 1024], P(None, 'tp'), may hold values from -0.125 to 0.125
- conv_kernel: bfloat16 [3, 1024], P(None, 'tp'), may hold values from -3 to 3
- group_gain: float32 [1024], P('tp'), may hold values from 0.1 to 1.9
- mixer_out_weight: bfloat16 [1024, 2048], P(None, 'tp'), may hold values from -0.1875 to 0.1875
- expert_input: bfloat16 [2048, 2048], P('ep'), may hold values from -6 to 6
- expert_gain: float32 [2048], replicated, may hold values from 0.1 to 1.9
- routes: int32 [2048, 2], P('ep'), may hold values from 0 to 7, all different within a row; in each aligned block of 256 rows (0 to 255, 256 to 511, ...) at most 128 rows name the same one
- route_weight: float32 [2048, 2], P('ep'), may hold values from 0.1 to 1
- expert_gate: bfloat16 [8, 2048, 3584], P('ep', None, 'tp'), may hold values from -0.125 to 0.125
- expert_up: bfloat16 [8, 2048, 3584], P('ep', None, 'tp'), may hold values from -0.125 to 0.125
- expert_down: bfloat16 [8, 3584, 2048], P('ep', None, 'tp'), may hold values from -0.09375 to 0.09375
Outputs:
- mixed_tokens: bfloat16 [1024, 2048], P('ep', 'tp')
- expert_tokens: bfloat16 [2048, 2048], P('ep', 'tp')
The draws below stay inside these ranges and needn't reach their ends.
Inputs may be any that keep to these rules, and one draw needn't show every extreme that they name: `routes`: each row names 2 different experts. Within the rows of one index of ep no expert is named by more than 128 rows, a bound that some block reaches of them.
All inputs are finite; a program needn't handle non-finite values.
Results may differ from the reference program's by a relative error of at most 0.014.
Values may be sent and summed in bfloat16 or wider, within the bound.
No kernel may reach another device: no remote copies, remote signals or barrier semaphores. Data moves between devices by JAX's collectives and lax.ppermute only.
A program may use at most 64 MiB of HBM per device.

```python
import math
import jax
import jax.numpy as jnp
import numpy as np
from jax import lax

D = 2048
CONV = 1024
GROUP = 64
FF = 3584
TOP = 2
EXP_ROWS = 256
EXPERTS = 8
CAP = 128
MIX_TOKENS = 1024
EXP_TOKENS = 2048
N_EP = 8


def level_of(rng, extent, cuts, smallest, high):
    loudness = 1.0
    for dim, blocks in cuts:
        draws = jax.random.uniform(jax.random.fold_in(jax.random.fold_in(rng, 6), dim), (blocks,), jnp.float32, smallest / len(cuts), high / len(cuts))
        loudness = loudness * jnp.repeat(jnp.exp(draws), extent[dim] // blocks).reshape((-1,) + (1,) * (len(extent) - 1 - dim))
    return loudness


def assign_block(own_key, own, number, rows, count, top, bound, skew):
    ranking = jax.random.permutation(own_key, count)
    packed, common = load_shares(count, rows * top, bound, skew, True), load_shares(count, rows * top, bound, skew, False)
    places = jnp.arange(count)

    def named(tallies, turn):
        used = int((tallies > 0).sum())
        fixed = max(1, used // 4)
        passed = fixed + (places - fixed + turn * (used - fixed)) % max(1, count - fixed)
        return jnp.zeros((count,), jnp.int32).at[ranking[jnp.where(places < fixed, places, passed)]].set(jnp.asarray(tallies, jnp.int32))

    tallies = jnp.where(number % 4 == 0, named(packed, number // 4), named(common, number - number // 4 - 1))
    mixed = jax.random.permutation(jax.random.fold_in(own, 3), count)
    source_of, taker = mixed[0:count // 2 * 2:2], mixed[1:count // 2 * 2:2]
    room = jnp.minimum(tallies[source_of] - 1, bound - tallies[taker]) // 2
    room = jnp.where((source_of == ranking[0]) | (taker == ranking[0]) | (tallies[taker] == 0), 0, jnp.maximum(room, 0))
    passed = jax.random.randint(jax.random.fold_in(own, 4), (count // 2,), 0, 1 << 20) % (room + 1)
    tallies = tallies.at[source_of].add(-passed).at[taker].add(passed)
    members = jnp.searchsorted(jnp.cumsum(tallies), jnp.arange(rows * top), side="right").astype(jnp.int32)
    table = members.reshape(top, rows).T
    table = table[jax.random.permutation(jax.random.fold_in(own, 1), rows)]
    turn = jax.random.randint(jax.random.fold_in(own, 2), (rows, 1), 0, top)
    return jnp.take_along_axis(table, (jnp.arange(top)[None, :] + turn) % top, axis=1)


def load_shares(count, total, most, skew, full):
    loads = [(1 << 20) // math.isqrt(rank ** skew) + 1 for rank in range(1, count + 1)]
    largest = most if full else min(most, max(-(-total // count), total * loads[0] // sum(loads)))
    least = 1 if total - largest >= count - 1 else 0
    holding, surplus = [largest] + [least] * (count - 1), total - largest - least * (count - 1)
    while surplus > 0:
        movable = [i for i in range(1, count) if holding[i] < largest] or [i for i in range(1, count) if holding[i] < most]
        whole, remaining = sum([loads[i] for i in movable]), surplus
        for i in movable:
            addition = min(most - holding[i], max(1, remaining * loads[i] // whole), surplus)
            holding[i] = holding[i] + addition
            surplus = surplus - addition
    return np.array(holding)


def scatter_about(stream_key, dims, spread, limit, shards=(), kind=jnp.bfloat16):
    values = spread * jax.random.normal(stream_key, dims, jnp.float32)
    if shards:
        values = values * level_of(stream_key, dims, shards, -0.22, 0.18)
    return jnp.clip(values, -limit, limit).astype(kind)


def setup_inputs(seed: int = 0) -> dict:
    splits = jax.random.split(jax.random.key(seed), 16)
    mixer_input = scatter_about(splits[0], (MIX_TOKENS, D), 1.0, 6.0, ((0, 8),))
    mixer_gain = jnp.clip(1.0 + 0.18 * jax.random.normal(splits[1], (D,), jnp.float32), 0.1, 1.9)
    outer_weight = scatter_about(splits[2], (D, CONV), D ** -0.5, 0.125, ((1, 4),))
    inner_weight = scatter_about(splits[3], (D, CONV), D ** -0.5, 0.125, ((1, 4),))
    value_weight = scatter_about(splits[4], (D, CONV), D ** -0.5, 0.125, ((1, 4),))
    conv_kernel = scatter_about(splits[5], (3, CONV), 0.6, 3.0, ((1, 4),))
    group_gain = jnp.clip(1.0 + 0.18 * jax.random.normal(splits[6], (CONV,), jnp.float32), 0.1, 1.9)
    mixer_out_weight = scatter_about(splits[7], (CONV, D), CONV ** -0.5, 0.1875, ((1, 4),))
    expert_input = scatter_about(splits[8], (EXP_TOKENS, D), 1.0, 6.0, ((0, 8),))
    expert_gain = jnp.clip(1.0 + 0.18 * jax.random.normal(splits[9], (D,), jnp.float32), 0.1, 1.9)
    routes_keys = jax.random.split(jax.random.fold_in(splits[10], 1), EXP_TOKENS // EXP_ROWS)
    routes_turns = jax.random.permutation(jax.random.fold_in(splits[10], 3), EXP_TOKENS // EXP_ROWS)
    routes = jax.vmap(lambda own, number: assign_block(jax.random.fold_in(splits[10], 2), own, number, EXP_ROWS, EXPERTS, TOP, CAP, 2))(routes_keys, routes_turns).reshape((EXP_TOKENS, TOP))
    route_weight = jnp.clip(0.1 + 0.9 * jax.random.uniform(splits[11], (EXP_TOKENS, TOP), jnp.float32) ** level_of(splits[11], (EXP_TOKENS, TOP), ((0, 8),), -0.2, 0.2), 0.1, 1.0)
    expert_gate = scatter_about(splits[12], (EXPERTS, D, FF), D ** -0.5, 0.125, ((0, 8), (2, 4)))
    expert_up = scatter_about(splits[13], (EXPERTS, D, FF), D ** -0.5, 0.125, ((0, 8), (2, 4)))
    expert_down = scatter_about(splits[14], (EXPERTS, FF, D), FF ** -0.5, 0.09375, ((0, 8), (2, 4)))
    return dict(mixer_input=mixer_input, mixer_gain=mixer_gain, outer_weight=outer_weight, inner_weight=inner_weight, value_weight=value_weight, conv_kernel=conv_kernel, group_gain=group_gain, mixer_out_weight=mixer_out_weight, expert_input=expert_input, expert_gain=expert_gain, routes=routes, route_weight=route_weight, expert_gate=expert_gate, expert_up=expert_up, expert_down=expert_down)


EPS = 1e-06

def rms_scale(values, gain):
    floats = values.astype(jnp.float32)
    scale = lax.rsqrt(lax.optimization_barrier(jnp.mean(floats * floats, axis=-1, keepdims=True)) + EPS)
    return floats * scale * gain.astype(jnp.float32)

def run_expert(operands):
    rows, gate_part, up_part, down_part = operands
    gate = jnp.dot(rows, gate_part, preferred_element_type=jnp.float32)
    up_value = jnp.dot(rows, up_part, preferred_element_type=jnp.float32)
    hidden = (jax.nn.silu(gate) * up_value).astype(jnp.bfloat16)
    return jnp.dot(hidden, down_part, preferred_element_type=jnp.float32).astype(jnp.bfloat16)

def reference(mixer_input, mixer_gain, outer_weight, inner_weight, value_weight, conv_kernel, group_gain, mixer_out_weight, expert_input, expert_gain, routes, route_weight, expert_gate, expert_up, expert_down):
    count = mixer_input.shape[0]
    normed_a = rms_scale(mixer_input, mixer_gain).astype(jnp.bfloat16)
    outer = jnp.dot(normed_a, outer_weight, preferred_element_type=jnp.float32).astype(jnp.bfloat16)
    inner = jnp.dot(normed_a, inner_weight, preferred_element_type=jnp.float32).astype(jnp.bfloat16)
    values = jnp.dot(normed_a, value_weight, preferred_element_type=jnp.float32).astype(jnp.bfloat16)
    product = inner.astype(jnp.float32) * values.astype(jnp.float32)
    padded = jnp.pad(product, ((2, 0), (0, 0)))
    kernel = conv_kernel.astype(jnp.float32)
    conv_sum = kernel[0] * padded[0:count] + kernel[1] * padded[1:count + 1] + kernel[2] * padded[2:count + 2]
    gated = outer.astype(jnp.float32) * conv_sum
    grouped = gated.reshape(count, CONV // GROUP, GROUP)
    grouped = rms_scale(grouped, group_gain.reshape(CONV // GROUP, GROUP))
    grouped = grouped.reshape(count, CONV).astype(jnp.bfloat16)
    mixed_tokens = jnp.dot(grouped, mixer_out_weight, preferred_element_type=jnp.float32).astype(jnp.bfloat16)
    normed_b = rms_scale(expert_input, expert_gain).astype(jnp.bfloat16)
    picks = routes.reshape(N_EP, EXP_ROWS * TOP).astype(jnp.int32)
    onehot = (picks[:, :, None] == jnp.arange(EXPERTS, dtype=jnp.int32)[None, None, :]).astype(jnp.int32)
    earlier = jnp.cumsum(onehot, axis=1) - onehot
    rank = lax.optimization_barrier(jnp.sum(earlier * onehot, axis=2)).astype(jnp.int32)
    slot = (picks * CAP + rank).astype(jnp.int32)
    token = (jnp.arange(EXP_ROWS * TOP, dtype=jnp.int32) // TOP).astype(jnp.int32)
    source = jnp.arange(N_EP, dtype=jnp.int32)[:, None]
    table = jnp.zeros((N_EP, EXPERTS * CAP), jnp.int32).at[source, slot].set(token[None, :] + 1)
    valid = table > 0
    row_index = (source * EXP_ROWS + jnp.maximum(table - 1, 0)).astype(jnp.int32)
    buffer = jnp.where(valid[..., None], jnp.take(normed_b, row_index, axis=0), 0).astype(jnp.bfloat16)
    per_expert = buffer.reshape(N_EP, EXPERTS, CAP, D).transpose(1, 0, 2, 3).reshape(EXPERTS, N_EP * CAP, D)
    outputs = lax.map(run_expert, (per_expert, expert_gate, expert_up, expert_down))
    flat_out = outputs.reshape(EXPERTS * N_EP * CAP, D)
    position = (picks * (N_EP * CAP) + source * CAP + rank).astype(jnp.int32)
    chosen = jnp.take(flat_out, position.reshape(-1), axis=0).astype(jnp.float32).reshape(N_EP * EXP_ROWS, TOP, D)
    weighted = lax.optimization_barrier(jnp.sum(chosen * route_weight.astype(jnp.float32)[..., None], axis=1))
    expert_tokens = weighted.astype(jnp.bfloat16)
    return (mixed_tokens, expert_tokens)
```

```python
import jax
import jax.numpy as jnp
from jax import lax
from jax.sharding import PartitionSpec as P

GROUP = 64
CHUNKS = 2


EPS = 1e-06


def from_behind(block, axis, distance):
    devices = range(lax.axis_size(axis))
    route = [(i - distance, i) for i in devices if i - distance in devices]
    return lax.ppermute(block, axis, route)


def rms_scale(values, gain):
    floats = values.astype(jnp.float32)
    scale = lax.rsqrt(jnp.mean(floats * floats, axis=-1, keepdims=True) + EPS)
    return floats * scale * gain


def per_device(
    mixer_input,
    mixer_gain,
    outer_weight,
    inner_weight,
    value_weight,
    conv_kernel,
    group_gain,
    mixer_out_weight,
    expert_input,
    expert_gain,
    routes,
    route_weight,
    expert_gate,
    expert_up,
    expert_down,
):
    mix_count = mixer_input.shape[0]
    normed_a = rms_scale(mixer_input, mixer_gain).astype(jnp.bfloat16)
    outer = jnp.dot(normed_a, outer_weight, preferred_element_type=jnp.float32).astype(jnp.bfloat16)
    inner = jnp.dot(normed_a, inner_weight, preferred_element_type=jnp.float32).astype(jnp.bfloat16)
    values = jnp.dot(normed_a, value_weight, preferred_element_type=jnp.float32).astype(
        jnp.bfloat16
    )
    product = inner.astype(jnp.float32) * values.astype(jnp.float32)
    earlier_rows = from_behind(product[mix_count - 2 :], "ep", 1)
    padded = jnp.concatenate([earlier_rows, product], axis=0)
    kernel = conv_kernel.astype(jnp.float32)
    conv_sum = (
        kernel[0] * padded[0:mix_count]
        + kernel[1] * padded[1 : mix_count + 1]
        + kernel[2] * padded[2 : mix_count + 2]
    )
    gated = outer.astype(jnp.float32) * conv_sum
    grouped = gated.reshape(mix_count, -1, GROUP)
    grouped = rms_scale(grouped, group_gain.reshape(-1, GROUP))
    grouped = grouped.reshape(mix_count, -1).astype(jnp.bfloat16)
    weight_rows = mixer_out_weight
    mixed_tokens = jnp.dot(
        lax.all_gather(grouped, "tp", axis=1, tiled=True),
        weight_rows,
        preferred_element_type=jnp.float32,
    ).astype(jnp.bfloat16)
    exp_count, picks_each = routes.shape
    width = expert_input.shape[1]
    experts = expert_gate.shape[0] * lax.axis_size("ep")
    capacity = 2 * picks_each * exp_count // experts
    parts = lax.axis_size("tp")
    part = lax.axis_index("tp")
    span = width // parts
    share = capacity // CHUNKS

    routes_t = routes.T
    ids = lax.broadcasted_iota(jnp.int32, (experts, exp_count), 0)
    hits = [routes_t[k : k + 1] == ids for k in range(picks_each)]
    named = hits[0]
    for hit in hits[1:]:
        named = named | hit
    ahead = lax.broadcasted_iota(jnp.int32, (exp_count, exp_count), 0) < lax.broadcasted_iota(
        jnp.int32, (exp_count, exp_count), 1
    )
    rank = jnp.dot(
        named.astype(jnp.bfloat16), ahead.astype(jnp.bfloat16), preferred_element_type=jnp.float32
    ).astype(jnp.int32)
    slots = [
        jnp.sum(jnp.where(hit, ids * capacity + rank, 0), axis=0, keepdims=True) for hit in hits
    ]

    floats = expert_input.astype(jnp.float32)
    scale = lax.rsqrt(jnp.mean(floats * floats, axis=-1, keepdims=True) + EPS)
    own_input = lax.dynamic_slice_in_dim(expert_input, part * span, span, 1).astype(jnp.float32)
    own_gain = lax.dynamic_slice_in_dim(expert_gain, part * span, span, 0)
    normed_b = (own_input * scale * own_gain).astype(jnp.bfloat16)

    gate_weight = expert_gate[0]
    up_weight = expert_up[0]
    down_weight = expert_down[0]
    out_cols = down_weight.shape[1]

    def spread(block):
        blocks = [(0, block)]
        step = parts // 2
        while step:
            pairs = [(i, i ^ step) for i in range(parts)]
            blocks = blocks + [(k ^ step, lax.ppermute(one, "tp", pairs)) for k, one in blocks]
            step //= 2
        return blocks

    def summed(blocks, weight):
        total = None
        for k, one in blocks:
            rows = one.shape[1]
            piece = lax.dynamic_slice_in_dim(weight, (part ^ k) * rows, rows, 0)
            term = jnp.dot(one, piece, preferred_element_type=jnp.float32)
            total = term if total is None else total + term
        return total

    def slot_ids(chunk, shape, axis):
        place = lax.broadcasted_iota(jnp.int32, shape, axis)
        return place // share * capacity + chunk * share + place % share

    chunk_rows = experts * share
    received = []
    for chunk in range(CHUNKS):
        wanted = slot_ids(chunk, (chunk_rows, exp_count), 0)
        chosen = wanted == slots[0]
        for slot in slots[1:]:
            chosen = chosen | (wanted == slot)
        outgoing = jnp.dot(
            chosen.astype(jnp.bfloat16), normed_b, preferred_element_type=jnp.float32
        ).astype(jnp.bfloat16)
        arrived = lax.all_to_all(
            outgoing.reshape(experts, share, span), "ep", split_axis=0, concat_axis=0, tiled=True
        )
        received.append(arrived.reshape(chunk_rows, span))

    picked = None
    slot_column = jnp.concatenate(slots, axis=1).reshape(-1, 1)
    for chunk in range(CHUNKS):
        blocks = spread(received[chunk])
        gate = summed(blocks, gate_weight)
        up_value = summed(blocks, up_weight)
        hidden = (jax.nn.silu(gate) * up_value).astype(jnp.bfloat16)
        results = summed(spread(hidden), down_weight).astype(jnp.bfloat16)
        returned = lax.all_to_all(
            results.reshape(experts, share, out_cols), "ep", split_axis=0, concat_axis=0, tiled=True
        ).reshape(chunk_rows, out_cols)
        taken = slot_column == slot_ids(chunk, (picks_each * exp_count, chunk_rows), 1)
        term = jnp.dot(taken.astype(jnp.bfloat16), returned, preferred_element_type=jnp.float32)
        picked = term if picked is None else picked + term
    picked = picked.reshape(picks_each, exp_count, out_cols)
    expert_tokens = jnp.sum(picked * route_weight.T[:, :, None], axis=0).astype(jnp.bfloat16)
    return (mixed_tokens, expert_tokens)


def solution(mesh):
    placed = (
        P("ep", None),
        P(),
        P(None, "tp"),
        P(None, "tp"),
        P(None, "tp"),
        P(None, "tp"),
        P("tp"),
        P(None, "tp"),
        P("ep", None),
        P(),
        P("ep", None),
        P("ep", None),
        P("ep", None, "tp"),
        P("ep", None, "tp"),
        P("ep", None, "tp"),
    )
    return jax.shard_map(
        per_device,
        mesh=mesh,
        in_specs=placed,
        out_specs=(P("ep", "tp"), P("ep", "tp")),
        check_vma=False,
    )
```

```python
import jax
import jax.numpy as jnp
from jax import lax
from jax.sharding import PartitionSpec as P


GROUP = 64
EIGHTHS = (2, 3, 3)


EPS = 1e-06


def from_behind(block, axis, distance):
    devices = range(lax.axis_size(axis))
    route = [(i - distance, i) for i in devices if i - distance in devices]
    return lax.ppermute(block, axis, route)


def rms_scale(values, gain):
    floats = values.astype(jnp.float32)
    scale = lax.rsqrt(jnp.mean(floats * floats, axis=-1, keepdims=True) + EPS)
    return floats * scale * gain


def per_device(
    mixer_input,
    mixer_gain,
    outer_weight,
    inner_weight,
    value_weight,
    conv_kernel,
    group_gain,
    mixer_out_weight,
    expert_input,
    expert_gain,
    routes,
    route_weight,
    expert_gate,
    expert_up,
    expert_down,
):
    mix_count = mixer_input.shape[0]
    normed_a = rms_scale(mixer_input, mixer_gain).astype(jnp.bfloat16)
    outer = jnp.dot(normed_a, outer_weight, preferred_element_type=jnp.float32).astype(jnp.bfloat16)
    inner = jnp.dot(normed_a, inner_weight, preferred_element_type=jnp.float32).astype(jnp.bfloat16)
    values = jnp.dot(normed_a, value_weight, preferred_element_type=jnp.float32).astype(
        jnp.bfloat16
    )
    product = inner.astype(jnp.float32) * values.astype(jnp.float32)
    earlier_rows = from_behind(product[mix_count - 2 :], "ep", 1)
    padded = jnp.concatenate([earlier_rows, product], axis=0)
    kernel = conv_kernel.astype(jnp.float32)
    conv_sum = (
        kernel[0] * padded[0:mix_count]
        + kernel[1] * padded[1 : mix_count + 1]
        + kernel[2] * padded[2 : mix_count + 2]
    )
    gated = outer.astype(jnp.float32) * conv_sum
    grouped = gated.reshape(mix_count, -1, GROUP)
    grouped = rms_scale(grouped, group_gain.reshape(-1, GROUP))
    grouped = grouped.reshape(mix_count, -1).astype(jnp.bfloat16)
    weight_rows = mixer_out_weight
    mixed_tokens = jnp.dot(
        lax.all_gather(grouped, "tp", axis=1, tiled=True),
        weight_rows,
        preferred_element_type=jnp.float32,
    ).astype(jnp.bfloat16)
    exp_count, picks_each = routes.shape
    width = expert_input.shape[1]
    experts = expert_gate.shape[0] * lax.axis_size("ep")
    capacity = 2 * picks_each * exp_count // experts
    parts = lax.axis_size("tp")
    part = lax.axis_index("tp")
    span = width // parts
    sizes = [capacity * eighths // sum(EIGHTHS) for eighths in EIGHTHS]
    starts = [sum(sizes[:chunk]) for chunk in range(len(sizes))]

    routes_t = routes.T
    ids = lax.broadcasted_iota(jnp.int32, (experts, exp_count), 0)
    hits = [routes_t[k : k + 1] == ids for k in range(picks_each)]
    named = hits[0]
    for hit in hits[1:]:
        named = named | hit
    ahead = lax.broadcasted_iota(jnp.int32, (exp_count, exp_count), 0) < lax.broadcasted_iota(
        jnp.int32, (exp_count, exp_count), 1
    )
    rank = jnp.dot(
        named.astype(jnp.bfloat16), ahead.astype(jnp.bfloat16), preferred_element_type=jnp.float32
    ).astype(jnp.int32)
    slots = [
        jnp.sum(jnp.where(hit, ids * capacity + rank, 0), axis=0, keepdims=True) for hit in hits
    ]

    floats = expert_input.astype(jnp.float32)
    scale = lax.rsqrt(jnp.mean(floats * floats, axis=-1, keepdims=True) + EPS)
    own_input = lax.dynamic_slice_in_dim(expert_input, part * span, span, 1).astype(jnp.float32)
    own_gain = lax.dynamic_slice_in_dim(expert_gain, part * span, span, 0)
    normed_b = (own_input * scale * own_gain).astype(jnp.bfloat16)

    gate_weight = expert_gate[0]
    up_weight = expert_up[0]
    down_weight = expert_down[0]
    out_cols = down_weight.shape[1]

    def spread(block):
        blocks = {0: block}
        step = parts // 2
        while step:
            pairs = [(i, i ^ step) for i in range(parts)]
            for k in list(blocks):
                blocks[k ^ step] = lax.ppermute(blocks[k], "tp", pairs)
            step //= 2
        return sorted(blocks.items())

    def summed(blocks, weight):
        total = None
        for k, one in blocks:
            rows = one.shape[1]
            piece = lax.dynamic_slice_in_dim(weight, (part ^ k) * rows, rows, 0)
            term = jnp.dot(one, piece, preferred_element_type=jnp.float32)
            total = term if total is None else total + term
        return total

    def slot_ids(chunk, shape, axis):
        place = lax.broadcasted_iota(jnp.int32, shape, axis)
        return place // sizes[chunk] * capacity + starts[chunk] + place % sizes[chunk]

    received = []
    for chunk, size in enumerate(sizes):
        wanted = slot_ids(chunk, (experts * size, exp_count), 0)
        chosen = wanted == slots[0]
        for slot in slots[1:]:
            chosen = chosen | (wanted == slot)
        outgoing = jnp.dot(
            chosen.astype(jnp.bfloat16), normed_b, preferred_element_type=jnp.float32
        ).astype(jnp.bfloat16)
        arrived = lax.all_to_all(
            outgoing.reshape(experts, size, span), "ep", split_axis=0, concat_axis=0, tiled=True
        )
        received.append(arrived.reshape(experts * size, span))

    picked = None
    slot_column = jnp.concatenate(slots, axis=1).reshape(-1, 1)
    for chunk, size in enumerate(sizes):
        blocks = spread(received[chunk])
        gate = summed(blocks, gate_weight)
        up_value = summed(blocks, up_weight)
        hidden = (jax.nn.silu(gate) * up_value).astype(jnp.bfloat16)
        results = summed(spread(hidden), down_weight).astype(jnp.bfloat16)
        returned = lax.all_to_all(
            results.reshape(experts, size, out_cols), "ep", split_axis=0, concat_axis=0, tiled=True
        )
        returned = returned.reshape(experts * size, out_cols)
        taken = slot_column == slot_ids(chunk, (picks_each * exp_count, experts * size), 1)
        term = jnp.dot(taken.astype(jnp.bfloat16), returned, preferred_element_type=jnp.float32)
        picked = term if picked is None else picked + term
    picked = picked.reshape(picks_each, exp_count, out_cols)
    expert_tokens = jnp.sum(picked * route_weight.T[:, :, None], axis=0).astype(jnp.bfloat16)
    return (mixed_tokens, expert_tokens)


def solution(mesh):
    placed = (
        P("ep", None),
        P(),
        P(None, "tp"),
        P(None, "tp"),
        P(None, "tp"),
        P(None, "tp"),
        P("tp"),
        P(None, "tp"),
        P("ep", None),
        P(),
        P("ep", None),
        P("ep", None),
        P("ep", None, "tp"),
        P("ep", None, "tp"),
        P("ep", None, "tp"),
    )

    return jax.shard_map(
        per_device,
        mesh=mesh,
        in_specs=placed,
        out_specs=(P("ep", "tp"), P("ep", "tp")),
        check_vma=False,
    )
```
